768 devices in a mesh: ep: 48 (over z, x), tp: 16 (over y, core).
Axes of the slice: x: 4, y: 8, z: 12, core: 2. Of those that a mesh axis runs over, the one named last changes fastest.
Arguments:
- tokens: bfloat16 [6144, 2048], P('ep'), may hold values from -6 to 6
- chosen: int32 [48, 48, 7], P('ep'), may hold values from -1 to 127, as said below
- pick_weight: float32 [48, 48, 7], P('ep'), may hold values from 0.2 to 1
- gate_weight: bfloat16 [48, 2048, 4096], P('ep', None, 'tp'), may hold values from -0.125 to 0.125
- up_weight: bfloat16 [48, 2048, 4096], P('ep', None, 'tp'), may hold values from -0.125 to 0.125
- down_weight: bfloat16 [48, 4096, 2048], P('ep', 'tp'), may hold values from -0.09375 to 0.09375
Outputs:
- combined: bfloat16 [6144, 2048], P('ep', 'tp')
The draws below stay inside these ranges and needn't reach their ends.
Inputs may be any that keep to these rules, and one draw needn't show every extreme that they name: `chosen`: within one group and one expert the named positions are distinct, and the filled slots come first. From each group every expert takes at least 3 tokens and at most 7; every expert takes exactly 7 tokens from some group, and exactly 240 tokens in all.
All inputs are finite; a program needn't handle non-finite values.
Results may differ from the reference program's by a relative error of at most 0.019.
Values may be sent and summed in bfloat16 or wider, within the bound.
A program may use at most 64 MiB of HBM per device.

```python
import math
import jax
import jax.numpy as jnp
from jax import lax

D = 2048
FF = 4096
TOK_DEV = 128
SLOTS = 7
PICK_DEV = 5
EXPERTS = 48
SOURCES = 48
TOKENS = 6144
N_TP = 16


def draw_chosen(key, part):
    key_count, key_order, key_tokens = jax.random.split(key, 3)
    half_count = SOURCES // 2
    spread = SLOTS - PICK_DEV
    excess = jax.random.randint(key_count, (EXPERTS, half_count), 0, spread + 1)
    excess = excess.at[:, 0].set(spread)
    signed = jnp.concatenate([excess, -excess], axis=1)
    shuffle = jax.vmap(lambda subkey: jax.random.permutation(subkey, SOURCES))(jax.random.split(key_order, EXPERTS))
    counts = PICK_DEV + jnp.take_along_axis(signed, shuffle, axis=1)
    counts = jnp.transpose(counts, (1, 0))
    token_keys = jax.random.split(key_tokens, SOURCES * EXPERTS)
    token_perm = jax.vmap(lambda subkey: jax.random.permutation(subkey, TOK_DEV)[:SLOTS])(token_keys)
    token_perm = token_perm.reshape(SOURCES, EXPERTS, SLOTS)
    slot_index = jnp.arange(SLOTS, dtype=jnp.int32)
    return jnp.where(slot_index[None, None, :] < counts[:, :, None], token_perm, -1).astype(jnp.int32)


def steps_of(rng, dims, pieces, least, top_value):
    def one(position, parts):
        draws = jax.random.uniform(jax.random.fold_in(jax.random.fold_in(rng, 6), position), (parts,), jnp.float32, least / len(pieces), top_value / len(pieces))
        return jnp.repeat(jnp.exp(draws), dims[position] // parts).reshape((-1,) + (1,) * (len(dims) - position - 1))

    loudness = one(*pieces[0])
    for cut in pieces[1:]:
        loudness = loudness * one(*cut)
    return loudness


def gaussian(stream_key, extent, scale, reach, shards=(), held_as=jnp.bfloat16):
    entries = jax.random.normal(stream_key, extent, jnp.float32) * scale
    if len(shards) > 0:
        entries = steps_of(stream_key, extent, shards, -0.22, 0.18) * entries
    return jnp.clip(entries, min=-reach, max=reach).astype(held_as)


def setup_inputs(seed: int = 0) -> dict:
    splits = jax.random.split(jax.random.key(seed), 7)
    tokens = gaussian(splits[0], (TOKENS, D), 1.0, 6.0, ((0, 48),))
    chosen = draw_chosen(jax.random.fold_in(splits[6], 71), 0)
    pick_weight = jnp.clip(jnp.exp(math.log(1.0) - 1.609438 * jax.random.uniform(splits[2], (SOURCES, EXPERTS, SLOTS), jnp.float32) ** steps_of(splits[2], (SOURCES, EXPERTS, SLOTS), ((0, 48),), -0.2, 0.2)), 0.2, 1.0)
    gate_weight = gaussian(splits[3], (EXPERTS, D, FF), D ** -0.5, 0.125, ((0, 48), (2, 16)))
    up_weight = gaussian(splits[4], (EXPERTS, D, FF), D ** -0.5, 0.125, ((0, 48), (2, 16)))
    down_weight = gaussian(splits[5], (EXPERTS, FF, D), FF ** -0.5, 0.09375, ((0, 48), (1, 16)))
    return {"tokens": tokens, "chosen": chosen, "pick_weight": pick_weight, "gate_weight": gate_weight, "up_weight": up_weight, "down_weight": down_weight}


def reference(tokens, chosen, pick_weight, gate_weight, up_weight, down_weight):
    filled = chosen >= 0
    offset = (jnp.arange(SOURCES, dtype=jnp.int32) * TOK_DEV)[:, None, None]
    row_ids = (jnp.where(filled, chosen, 0) + offset).astype(jnp.int32)
    row_ids = jnp.transpose(row_ids, (1, 0, 2)).reshape(EXPERTS, SOURCES * SLOTS)
    filled_flat = jnp.transpose(filled, (1, 0, 2)).reshape(EXPERTS, SOURCES * SLOTS)
    block_len = FF // N_TP

    def expert_step(inputs):
        expert_ids, keep_flags, w_gate, w_up, w_down = inputs
        routed = jnp.where(keep_flags[:, None], tokens[expert_ids], jnp.zeros((), tokens.dtype))
        gate_pre = jnp.dot(routed, w_gate, preferred_element_type=jnp.float32)
        up_pre = jnp.dot(routed, w_up, preferred_element_type=jnp.float32)
        hidden = (jax.nn.silu(gate_pre) * up_pre).astype(jnp.bfloat16)
        hidden = lax.optimization_barrier(hidden)
        hidden_wide = hidden.astype(jnp.float32).reshape(-1, N_TP, block_len)
        down_wide = w_down.astype(jnp.float32).reshape(N_TP, block_len, D)
        partial_value = jnp.einsum('rnf,nfd->nrd', hidden_wide, down_wide).astype(jnp.bfloat16)
        partial_value = lax.optimization_barrier(partial_value)
        return jnp.sum(partial_value.astype(jnp.float32), axis=0).astype(jnp.bfloat16)

    results = lax.map(expert_step, (row_ids, filled_flat, gate_weight, up_weight, down_weight))
    weights = jnp.where(filled_flat, jnp.transpose(pick_weight, (1, 0, 2)).reshape(EXPERTS, SOURCES * SLOTS), jnp.zeros((), jnp.float32))
    terms = weights.reshape(-1)[:, None] * results.reshape(-1, D).astype(jnp.float32)
    combined = jnp.zeros((TOKENS, D), jnp.float32).at[row_ids.reshape(-1)].add(terms)
    return combined.astype(jnp.bfloat16)
```

```python
import functools

import jax
import jax.numpy as jnp
from jax import lax
from jax.experimental import pallas as pl
from jax.experimental.pallas import tpu as pltpu
from jax.sharding import PartitionSpec as P

MESH = pl.DeviceIdType.MESH
F32 = jnp.float32
BF16 = jnp.bfloat16
LANES = 128
PAD = 8


def dot(a, b, dims=((1,), (0,))):
    return lax.dot_general(a, b, (dims, ((), ())), preferred_element_type=F32)


def iota(shape, dim):
    return lax.broadcasted_iota(jnp.int32, shape, dim)


def kernel(
    experts, x_size, y_size, cap, slots,
    tokens_ref, chosen_ref, pick_ref, gate_ref, up_ref, down_ref, out_ref,
    tok_v, pad_v, wgu, wd_own, wd_peer, low, sel_hi, sel_lo, spread,
    sbuf, rbuf, sbuf2, rbuf2, xo, xp, acc, hid_own, hid_peer, part, rs_out, rs_in, ysum,
    tok_sem, wgu_sem, wd_sem, wdp_send, wdp_recv, a1_send, a1_recv, a2_send, a2_recv,
    ag_send, ag_recv, dd_send, dd_recv, hid_send, hid_recv, rs_send, rs_recv,
):
    ep = lax.axis_index("ep")
    tp = lax.axis_index("tp")
    z_size = experts // x_size
    z, x = lax.div(ep, x_size), lax.rem(ep, x_size)
    y, core = lax.div(tp, 2), lax.rem(tp, 2)
    rows = experts * PAD
    half = cap // 2 // 16 * 16
    half = cap - half if cap - half <= LANES else half
    spans = ((0, half), (half, cap - half))
    ffd = gate_ref.shape[2]
    depth = tokens_ref.shape[0]

    def chip(rel):
        return lax.rem(y + rel + y_size, y_size)

    def far_first(i, size):
        return size // 2 + ((i + 1) // 2) * (1 - 2 * (i % 2))

    def ep_peer(i):
        dz = far_first(lax.div(i, x_size), z_size)
        dx = far_first(lax.rem(i, x_size), x_size)
        return lax.rem(z + dz, z_size) * x_size + lax.rem(x + dx, x_size)

    peer = (ep, tp + 1 - 2 * core)
    ring = {1: (ep, chip(1) * 2 + core), -1: (ep, chip(-1) * 2 + core)}

    barrier = pltpu.get_barrier_semaphore()

    def greet(i, carry):
        pl.semaphore_signal(barrier, inc=1, device_id=(ep_peer(i), tp), device_id_type=MESH)
        return carry

    lax.fori_loop(0, experts - 1, greet, 0)
    for other in (peer, ring[1], ring[-1]):
        pl.semaphore_signal(barrier, inc=1, device_id=other, device_id_type=MESH)

    tok_copy = pltpu.make_async_copy(
        tokens_ref.at[:, pl.ds(pl.multiple_of(tp * LANES, LANES), LANES)], tok_v, tok_sem
    )
    tok_copy.start()
    order = [0]
    for k in range(1, y_size // 2):
        order += [-k, k]
    order.append(y_size // 2)
    slot_of = {rel: j for j, rel in enumerate(order)}
    slot_of[-(y_size // 2)] = slot_of[y_size // 2]
    for j, rel in enumerate(order):
        for side in range(2):
            lane_block = chip(rel) * 2 + (core if side == 0 else 1 - core)
            src = pl.ds(pl.multiple_of(lane_block * LANES, LANES), LANES)
            dst = pl.ds(j * 2 * LANES + side * LANES, LANES)
            for n, w_ref in enumerate((gate_ref, up_ref)):
                pltpu.make_async_copy(
                    w_ref.at[0, src, :], wgu.at[dst, pl.ds(n * ffd, ffd)], wgu_sem
                ).start()
    back = order[::-1]
    for j, rel in enumerate(back):
        cols = pl.ds(pl.multiple_of((chip(rel) * 2 + core) * LANES, LANES), LANES)
        pltpu.make_async_copy(
            down_ref.at[0, :, cols], wd_own.at[:, pl.ds(j * LANES, LANES)], wd_sem
        ).start()

    pad_v[0] = jnp.full((experts, LANES), -1.0, F32)
    pad_v[1] = jnp.zeros((experts, LANES), F32)
    pad_v[0, :, 0:slots] = chosen_ref[0].astype(F32)
    pad_v[1, :, 0:slots] = pick_ref[0]
    row_expert = (iota((rows, experts), 0) // PAD == iota((rows, experts), 1)).astype(BF16)
    row_slot = iota((rows, LANES), 0) % PAD
    lane = iota((rows, LANES), 1)
    ones = jnp.ones((LANES, LANES), BF16)
    mine = row_slot == lane
    named = dot(row_expert, pad_v[0].astype(BF16))
    token_of = dot(jnp.where(mine, named, 0.0).astype(BF16), ones)
    count = dot((named >= 0.0).astype(F32).astype(BF16), ones)
    chosen_here = (token_of.astype(jnp.int32) == lane) & (row_slot < slots)
    pick_one = jnp.where(chosen_here, 1.0, 0.0)
    tok_copy.wait()
    message = dot(pick_one.astype(BF16), tok_v[...])
    message = jnp.where(row_slot == PAD - 1, count, message)
    sbuf[...] = message.reshape(experts, PAD, LANES).astype(BF16)
    rbuf[ep] = sbuf[ep]

    pl.semaphore_wait(barrier, experts - 1 + 3)

    def exchange(src, dst, send_sem, recv_sem):
        def send(i, carry):
            other = ep_peer(i)
            pltpu.make_async_remote_copy(
                src_ref=src.at[other], dst_ref=dst.at[ep], send_sem=send_sem, recv_sem=recv_sem,
                device_id=(other, tp), device_id_type=MESH,
            ).start()
            return carry

        lax.fori_loop(0, experts - 1, send, 0)

    def exchanged(ref, sem):
        some = ref.at[pl.ds(0, experts - 1)]
        pltpu.make_async_copy(some, some, sem).wait()

    exchange(sbuf, rbuf, a1_send, a1_recv)

    for j, rel in enumerate(back):
        cols = pl.ds(pl.multiple_of((chip(rel) * 2 + 1 - core) * LANES, LANES), LANES)
        pltpu.make_async_remote_copy(
            src_ref=down_ref.at[0, :, cols], dst_ref=wd_peer.at[:, pl.ds(j * LANES, LANES)],
            send_sem=wdp_send, recv_sem=wdp_recv, device_id=peer, device_id_type=MESH,
        ).start()

    from_row = iota((rows, rows), 0)
    to_row = iota((rows, rows), 1)
    counts_row = from_row % PAD == PAD - 1
    low[:, 0:rows] = (counts_row & (from_row // PAD < to_row // PAD)).astype(F32).astype(BF16)
    low[:, rows : 2 * rows] = (
        counts_row & (from_row // PAD <= to_row // PAD)
    ).astype(F32).astype(BF16)
    weight = pad_v[1]
    weight_hi = weight.astype(BF16)
    weight_lo = (weight - weight_hi.astype(F32)).astype(BF16)
    for table, piece in ((sel_hi, weight_hi), (sel_lo, weight_lo)):
        spread_out = jnp.where(mine, dot(row_expert, piece), 0.0).astype(BF16)
        table[...] = jnp.transpose(dot(spread_out, ones) * pick_one).astype(BF16)
    acc[...] = jnp.zeros_like(acc)
    ysum[...] = jnp.zeros_like(ysum)

    exchanged(rbuf, a1_recv)
    arrived = rbuf[...].astype(F32).reshape(rows, LANES).astype(BF16)
    bounds = dot(arrived, low[...], ((0,), (0,)))
    first, end = bounds[:, 0:rows].astype(jnp.int32), bounds[:, rows : 2 * rows].astype(jnp.int32)
    slot_row = iota((LANES, rows), 1) % PAD
    places = []

    def ag_copy(sign, part_id, k):
        lo, size = spans[part_id]
        window = pl.ds(lo, size)
        index = ((0 if sign > 0 else 1) * 2 + part_id) * (y_size // 2) + k - 1
        return pltpu.make_async_remote_copy(
            src_ref=xo.at[slot_of[-sign * (k - 1)], window, :],
            dst_ref=xo.at[slot_of[-sign * k], window, :],
            send_sem=ag_send.at[index], recv_sem=ag_recv.at[index],
            device_id=ring[sign], device_id_type=MESH,
        )

    def dd_copy(j, part_id):
        lo, size = spans[part_id]
        window = pl.ds(lo, size)
        return pltpu.make_async_remote_copy(
            src_ref=xo.at[j, window, :], dst_ref=xp.at[j, window, :],
            send_sem=dd_send.at[j * 2 + part_id], recv_sem=dd_recv.at[j * 2 + part_id],
            device_id=peer, device_id_type=MESH,
        )

    last = {(1, 0): y_size // 2, (1, 1): y_size // 2 - 1, (-1, 1): y_size // 2, (-1, 0): y_size // 2 - 1}
    started = []

    def go(copy):
        copy.start()
        started.append(copy)

    for part_id, (lo, size) in enumerate(spans):
        base = iota((LANES, rows), 0) + lo
        here = (first + slot_row == base) & (base < end)
        if size < LANES:
            here = here & (base < lo + size)
        place = jnp.where(here, 1.0, 0.0)
        places.append(place)
        xo[0, lo : lo + size, :] = dot(place.astype(BF16), arrived)[0:size].astype(BF16)
        for sign in (1, -1):
            go(ag_copy(sign, part_id, 1))
        go(dd_copy(0, part_id))
    for part_id, (lo, size) in enumerate(spans):
        spread[part_id] = jnp.transpose(places[part_id]).astype(BF16)

    pltpu.make_async_copy(wgu, wgu, wgu_sem).wait()

    def multiply(rel):
        j = slot_of[rel]
        for part_id in range(2):
            dd_copy(j, part_id).wait_recv()
        lhs = jnp.concatenate([xo[j], xp[j]], axis=1)
        acc[...] += dot(lhs, wgu[j * 2 * LANES : (j + 1) * 2 * LANES, :])

    for k in range(1, y_size // 2 + 1):
        if k == 1:
            multiply(0)
        for sign, part_id in ((1, 0), (-1, 1), (1, 1), (-1, 0)):
            if k > last[sign, part_id]:
                continue
            ag_copy(sign, part_id, k).wait_recv()
            if k < last[sign, part_id]:
                go(ag_copy(sign, part_id, k + 1))
            go(dd_copy(slot_of[-sign * k], part_id))
        if k > 1:
            multiply(-(k - 1))
            multiply(k - 1)
    multiply(y_size // 2)

    gate, up = acc[:, 0:ffd], acc[:, ffd : 2 * ffd]
    hid_own[...] = (gate / (1.0 + jnp.exp(-gate)) * up).astype(BF16)
    hid_copy = pltpu.make_async_remote_copy(
        src_ref=hid_own, dst_ref=hid_peer, send_sem=hid_send, recv_sem=hid_recv,
        device_id=peer, device_id_type=MESH,
    )
    go(hid_copy)
    pltpu.make_async_copy(wd_own, wd_own, wd_sem).wait()
    part[...] = dot(hid_own[...], wd_own[...])
    pltpu.make_async_copy(wd_peer, wd_peer, wdp_recv).wait()
    hid_copy.wait_recv()

    block_of = {rel: j for j, rel in enumerate(back)}
    block_of[-(y_size // 2)] = 0

    def rs_index(sign, part_id, k):
        return ((0 if sign > 0 else 1) * 2 + part_id) * (y_size // 2) + k - 1

    def rs_copy(sign, part_id, k):
        index = rs_index(sign, part_id, k)
        window = pl.ds(0, spans[part_id][1])
        return pltpu.make_async_remote_copy(
            src_ref=rs_out.at[index, window, :], dst_ref=rs_in.at[index, window, :],
            send_sem=rs_send.at[index], recv_sem=rs_recv.at[index],
            device_id=ring[sign], device_id_type=MESH,
        )

    def own(rel, part_id):
        lo, size = spans[part_id]
        j = block_of[rel]
        return part[lo : lo + size, j * LANES : (j + 1) * LANES]

    def rs_step(sign, part_id, k):
        rel = sign * (last[sign, part_id] + 1 - k)
        total = own(rel, part_id)
        size = spans[part_id][1]
        if k > 1:
            rs_copy(sign, part_id, k - 1).wait_recv()
            total += rs_in[rs_index(sign, part_id, k - 1), 0:size, :].astype(F32)
        rs_out[rs_index(sign, part_id, k), 0:size, :] = total.astype(BF16)
        go(rs_copy(sign, part_id, k))

    def add_peer(j, count):
        cols = slice(j * LANES, (j + count) * LANES)
        part[:, cols] += dot(hid_peer[...], wd_peer[:, cols])

    add_peer(0, 1)
    rs_step(1, 0, 1)
    rs_step(-1, 1, 1)
    add_peer(1, 2)
    rs_step(1, 1, 1)
    rs_step(-1, 0, 1)
    add_peer(3, y_size - 3)
    for k in range(2, y_size // 2 + 1):
        for sign, part_id in ((1, 0), (-1, 1), (1, 1), (-1, 0)):
            if k <= last[sign, part_id]:
                rs_step(sign, part_id, k)
    for part_id, (lo, size) in enumerate(spans):
        total = own(0, part_id)
        for sign in (1, -1) if part_id == 1 else (-1, 1):
            k = last[sign, part_id]
            rs_copy(sign, part_id, k).wait_recv()
            total += rs_in[rs_index(sign, part_id, k), 0:size, :].astype(F32)
        ysum[part_id, 0:size, :] = total.astype(BF16)

    result = dot(spread[0], ysum[0]) + dot(spread[1], ysum[1])
    sbuf2[...] = result.reshape(experts, PAD, LANES).astype(BF16)
    exchange(sbuf2, rbuf2, a2_send, a2_recv)
    rbuf2[ep] = sbuf2[ep]
    exchanged(rbuf2, a2_recv)
    got = rbuf2[...].astype(F32).reshape(rows, LANES).astype(BF16)
    out_ref[...] = (dot(sel_hi[...], got) + dot(sel_lo[...], got)).astype(out_ref.dtype)

    for copy in started:
        copy.wait_send()
    exchanged(sbuf, a1_send)
    exchanged(sbuf2, a2_send)
    pltpu.make_async_copy(wd_peer, wd_peer, wdp_send).wait()


def on_device(experts, x_size, y_size, cap, tokens, chosen, pick_weight, gate_weight, up_weight, down_weight):
    depth, width = tokens.shape
    slots = chosen.shape[2]
    ffd = gate_weight.shape[2]
    rows = experts * PAD
    messages = 4 * (y_size // 2)
    dma = pltpu.SemaphoreType.DMA
    hbm = pl.BlockSpec(memory_space=pltpu.MemorySpace.HBM)
    vmem = pl.BlockSpec(memory_space=pltpu.MemorySpace.VMEM)
    return pl.pallas_call(
        functools.partial(kernel, experts, x_size, y_size, cap, slots),
        out_shape=jax.ShapeDtypeStruct((depth, LANES), BF16),
        in_specs=[hbm, vmem, vmem, hbm, hbm, hbm],
        out_specs=vmem,
        scratch_shapes=[
            pltpu.VMEM((depth, LANES), BF16),
            pltpu.VMEM((2, experts, LANES), F32),
            pltpu.VMEM((width, 2 * ffd), BF16),
            pltpu.VMEM((ffd, y_size * LANES), BF16),
            pltpu.VMEM((ffd, y_size * LANES), BF16),
            pltpu.VMEM((rows, 2 * rows), BF16),
            pltpu.VMEM((depth, rows), BF16),
            pltpu.VMEM((depth, rows), BF16),
            pltpu.VMEM((2, rows, LANES), BF16),
            pltpu.VMEM((experts, PAD, LANES), BF16),
            pltpu.VMEM((experts, PAD, LANES), BF16),
            pltpu.VMEM((experts, PAD, LANES), BF16),
            pltpu.VMEM((experts, PAD, LANES), BF16),
            pltpu.VMEM((y_size, cap, LANES), BF16),
            pltpu.VMEM((y_size, cap, LANES), BF16),
            pltpu.VMEM((cap, 2 * ffd), F32),
            pltpu.VMEM((cap, ffd), BF16),
            pltpu.VMEM((cap, ffd), BF16),
            pltpu.VMEM((cap, y_size * LANES), F32),
            pltpu.VMEM((messages, LANES, LANES), BF16),
            pltpu.VMEM((messages, LANES, LANES), BF16),
            pltpu.VMEM((2, LANES, LANES), BF16),
            dma, dma, dma, dma, dma, dma, dma, dma, dma,
            dma((messages,)), dma((messages,)),
            dma((2 * y_size,)), dma((2 * y_size,)),
            dma, dma,
            dma((messages,)), dma((messages,)),
        ],
        compiler_params=pltpu.CompilerParams(collective_id=0, has_side_effects=True),
        name="experts",
    )(tokens, chosen, pick_weight, gate_weight, up_weight, down_weight)


def solution(mesh, x_size=4, cap=240):
    experts, tp = mesh.shape["ep"], mesh.shape["tp"]
    return jax.shard_map(
        functools.partial(on_device, experts, x_size, tp // 2, cap),
        mesh=mesh,
        in_specs=(
            P("ep", None),
            P("ep", None, None),
            P("ep", None, None),
            P("ep", None, "tp"),
            P("ep", None, "tp"),
            P("ep", "tp", None),
        ),
        out_specs=P("ep", "tp"),
        check_vma=False,
    )
```
